32 devices in a mesh: rep: 2 (over x), fs: 8 (over z, y), tp: 2 (over core).
Axes of the slice: x: 2, y: 2, z: 4, core: 2. Of those that a mesh axis runs over, the one named last changes fastest.
Arguments:
- tokens: bfloat16 [2048, 2048], P(('rep', 'fs')), may hold values from -6 to 6
- attention_norm_gain: float32 [2048], replicated, may hold values from 0.1 to 1.9
- query_weight: bfloat16 [2048, 1024], P('fs', 'tp'), may hold values from -0.125 to 0.125
- key_weight: bfloat16 [2048, 1024], P('fs', 'tp'), may hold values from -0.125 to 0.125
- value_weight: bfloat16 [2048, 2048], P('fs', 'tp'), may hold values from -0.125 to 0.125
- decay_weight: bfloat16 [2048, 1024], P('fs', 'tp'), may hold values from -0.125 to 0.125
- decay_gate_bias: float32 [1024], P('tp'), may hold values from -1.5 to 5.5
- decay_spike_extra: float32 [2048, 32], P(('rep', 'fs'), 'tp'), may hold values from -0.7 to 0
- head_output_gain: float32 [64], replicated, may hold values from 0.1 to 1.9
- output_weight: bfloat16 [2048, 2048], P('fs', 'tp'), may hold values from -0.125 to 0.125
- channel_norm_gain: float32 [2048], replicated, may hold values from 0.1 to 1.9
- gate_weight: bfloat16 [2048, 3072], P('fs', 'tp'), may hold values from -0.125 to 0.125
- up_weight: bfloat16 [2048, 3072], P('fs', 'tp'), may hold values from -0.125 to 0.125
- down_weight: bfloat16 [2048, 3072], P('fs', 'tp'), may hold values from -0.109375 to 0.109375
Outputs:
- layer_out: bfloat16 [2048, 2048], P(('rep', 'fs'))
The draws below stay inside these ranges and needn't reach their ends.
All inputs are finite; a program needn't handle non-finite values.
Results may differ from the reference program's by a relative error of at most 0.018.
Values may be sent and summed in bfloat16 or wider, within the bound.
A program may use at most 128 MiB of HBM per device.

```python
import jax
import jax.numpy as jnp
from jax import lax

D = 2048
HEAD_K = 32
HEAD_V = 64
HEADS = 32
FF = 3072
BLOCK = 64
TOK_GROUP = 128
TOKENS = 2048
N_TP = 2


def draw_decay_gate_bias(key, part):
    keys_all = jax.random.split(key, 4)
    fast_share = 0.5
    is_fast = jax.random.uniform(keys_all[0], (HEADS,), jnp.float32) < fast_share
    fast_value = jax.random.uniform(keys_all[1], (HEADS,), jnp.float32, -1.0, 0.0)
    slow_value = jax.random.uniform(keys_all[2], (HEADS,), jnp.float32, 3.0, 5.0)
    base_value = jnp.where(is_fast, fast_value, slow_value)
    jitter = jax.random.uniform(keys_all[3], (HEADS, HEAD_K), jnp.float32, -0.5, 0.5)
    return (base_value[:, None] + jitter).reshape(HEADS * HEAD_K).astype(jnp.float32)


def draw_decay_spike_extra(key, part):
    keys_all = jax.random.split(key, 2)
    chosen = jax.random.uniform(keys_all[0], (TOKENS, HEADS), jnp.float32) < 3.0 / TOK_GROUP
    depth = jax.random.uniform(keys_all[1], (TOKENS, HEADS), jnp.float32, -0.7, -0.22)
    return jnp.where(chosen, depth, 0.0).astype(jnp.float32)


def levels(own_key, extent, cuts, smallest, high):
    loudness, own = 1.0, jax.random.fold_in(own_key, 6)
    for position, blocks in cuts:
        draws = jnp.exp(jax.random.uniform(jax.random.fold_in(own, position), (blocks,), jnp.float32, smallest / len(cuts), high / len(cuts)))
        loudness = loudness * jnp.repeat(draws, extent[position] // blocks).reshape([-1 if axis == position else 1 for axis in range(len(extent))])
    return loudness


def bell_draw(own_key, extent, deviation, bound, shards=(), kind=jnp.bfloat16):
    values = deviation * jax.random.normal(own_key, extent, jnp.float32)
    if shards:
        values = values * levels(own_key, extent, shards, -0.22, 0.18)
    return jnp.clip(values, -bound, bound).astype(kind)


def setup_inputs(seed: int = 0) -> dict:
    seeds = jax.random.split(jax.random.key(seed), 15)
    return {
        "tokens": bell_draw(seeds[0], (TOKENS, D), 1.0, 6.0, ((0, 16),)),
        "attention_norm_gain": jnp.clip(1.0 + 0.18 * jax.random.normal(seeds[1], (D,), jnp.float32), 0.1, 1.9),
        "query_weight": bell_draw(seeds[2], (D, HEADS * HEAD_K), D ** -0.5, 0.125, ((0, 8), (1, 2))),
        "key_weight": bell_draw(seeds[3], (D, HEADS * HEAD_K), D ** -0.5, 0.125, ((0, 8), (1, 2))),
        "value_weight": bell_draw(seeds[4], (D, HEADS * HEAD_V), D ** -0.5, 0.125, ((0, 8), (1, 2))),
        "decay_weight": bell_draw(seeds[5], (D, HEADS * HEAD_K), D ** -0.5, 0.125, ((0, 8), (1, 2))),
        "decay_gate_bias": draw_decay_gate_bias(jax.random.fold_in(seeds[14], 71), 0),
        "decay_spike_extra": draw_decay_spike_extra(jax.random.fold_in(seeds[14], 71), 0),
        "head_output_gain": jnp.clip(1.0 + 0.18 * jax.random.normal(seeds[8], (HEAD_V,), jnp.float32), 0.1, 1.9),
        "output_weight": bell_draw(seeds[9], (D, HEADS * HEAD_V), (HEADS * HEAD_V) ** -0.5, 0.125, ((0, 8), (1, 2))),
        "channel_norm_gain": jnp.clip(1.0 + 0.18 * jax.random.normal(seeds[10], (D,), jnp.float32), 0.1, 1.9),
        "gate_weight": bell_draw(seeds[11], (D, FF), D ** -0.5, 0.125, ((0, 8), (1, 2))),
        "up_weight": bell_draw(seeds[12], (D, FF), D ** -0.5, 0.125, ((0, 8), (1, 2))),
        "down_weight": bell_draw(seeds[13], (D, FF), FF ** -0.5, 0.109375, ((0, 8), (1, 2))),
    }


GATE_NORM = 16.0
NORM_EPS = 1e-06
HIGHEST = lax.Precision.HIGHEST

def rms_scale(values, scales):
    floats = values.astype(jnp.float32)
    return floats * lax.rsqrt(lax.optimization_barrier(jnp.mean(floats * floats, axis=-1, keepdims=True)) + NORM_EPS) * scales

def one_way(queries, key_rows, value_rows, decay_logarithm):
    length, number_of_heads, key_width = queries.shape
    value_width = value_rows.shape[2]
    block_count = length // BLOCK

    def blocks(tensor):
        return tensor.reshape(block_count, BLOCK, number_of_heads, tensor.shape[2]).transpose(0, 2, 1, 3)
    lower_mask = jnp.tril(jnp.ones((BLOCK, BLOCK), bool))

    def advance(carried, pieces):
        query_part, key_part, value_part, decay_part = pieces
        running = jnp.cumsum(decay_part, axis=1)
        spread = jnp.where(lower_mask[None, :, :, None], running[:, :, None, :] - running[:, None, :, :], -jnp.inf)
        scores = jnp.einsum('hid,hjd,hijd->hij', query_part, key_part, jnp.exp(spread), precision=HIGHEST)
        block_end = running[:, -1:, :]
        result = jnp.einsum('hij,hje->hie', scores, value_part, precision=HIGHEST)
        result = result + jnp.einsum('hid,hde->hie', query_part * jnp.exp(running), carried, precision=HIGHEST)
        carried = jnp.exp(block_end)[:, 0, :, None] * carried + jnp.einsum('hjd,hje->hde', key_part * jnp.exp(block_end - running), value_part, precision=HIGHEST)
        return (carried, result)
    zero_state = jnp.zeros((number_of_heads, key_width, value_width), jnp.float32)
    _, outputs = lax.scan(advance, zero_state, (blocks(queries), blocks(key_rows), blocks(value_rows), blocks(decay_logarithm)))
    return outputs.transpose(0, 2, 1, 3).reshape(length, number_of_heads, value_width)

def both_ways(queries, key_rows, value_rows, decay_logarithm):
    forward = one_way(queries, key_rows, value_rows, decay_logarithm)
    backward = one_way(jnp.flip(queries, 0), jnp.flip(key_rows, 0), jnp.flip(value_rows, 0), jnp.flip(decay_logarithm, 0))
    return forward + jnp.flip(backward, 0)

def rounded(floats):
    return lax.optimization_barrier(floats.astype(jnp.bfloat16)).astype(jnp.float32)

def grouped_sum(left, right):
    width = left.shape[1] // N_TP
    total = jnp.zeros((left.shape[0], right.shape[0]), jnp.float32)
    for shard_id in range(N_TP):
        part_left = left[:, shard_id * width:(shard_id + 1) * width]
        part_right = right[:, shard_id * width:(shard_id + 1) * width]
        partial_sum = lax.dot_general(part_left, part_right, (((1,), (1,)), ((), ())), preferred_element_type=jnp.float32)
        total = total + rounded(partial_sum)
    return total

def reference(tokens, attention_norm_gain, query_weight, key_weight, value_weight, decay_weight, decay_gate_bias, decay_spike_extra, head_output_gain, output_weight, channel_norm_gain, gate_weight, up_weight, down_weight):
    normed = rms_scale(tokens, attention_norm_gain).astype(jnp.bfloat16)
    queries = jnp.dot(normed, query_weight, preferred_element_type=jnp.float32).astype(jnp.bfloat16)
    key_rows = jnp.dot(normed, key_weight, preferred_element_type=jnp.float32).astype(jnp.bfloat16)
    value_rows = jnp.dot(normed, value_weight, preferred_element_type=jnp.float32).astype(jnp.bfloat16)
    gate_pre = jnp.dot(normed, decay_weight, preferred_element_type=jnp.float32)
    decay_logarithm = jax.nn.log_sigmoid(gate_pre + decay_gate_bias).reshape(TOKENS, HEADS, HEAD_K) / GATE_NORM
    decay_logarithm = decay_logarithm + decay_spike_extra[:, :, None]
    seq_count = TOKENS // TOK_GROUP
    query_seq = (queries.astype(jnp.float32) * HEAD_K ** (-0.5)).reshape(seq_count, TOK_GROUP, HEADS, HEAD_K)
    key_seq = key_rows.astype(jnp.float32).reshape(seq_count, TOK_GROUP, HEADS, HEAD_K)
    value_seq = value_rows.astype(jnp.float32).reshape(seq_count, TOK_GROUP, HEADS, HEAD_V)
    decay_seq = decay_logarithm.reshape(seq_count, TOK_GROUP, HEADS, HEAD_K)

    def attend(pieces):
        mixed_heads = both_ways(*pieces)
        normed_heads = rms_scale(mixed_heads, head_output_gain)
        return normed_heads.reshape(TOK_GROUP, HEADS * HEAD_V).astype(jnp.bfloat16)
    attended = lax.map(attend, (query_seq, key_seq, value_seq, decay_seq)).reshape(TOKENS, HEADS * HEAD_V)
    residual = (tokens.astype(jnp.float32) + grouped_sum(attended, output_weight)).astype(jnp.bfloat16)
    normed_two = rms_scale(residual, channel_norm_gain).astype(jnp.bfloat16)
    gate_pre_two = jnp.dot(normed_two, gate_weight, preferred_element_type=jnp.float32)
    up_proj = jnp.dot(normed_two, up_weight, preferred_element_type=jnp.float32)
    hidden = (jax.nn.silu(gate_pre_two) * up_proj).astype(jnp.bfloat16)
    return (residual.astype(jnp.float32) + grouped_sum(hidden, down_weight)).astype(jnp.bfloat16)
```

```python
import functools

import jax
import jax.numpy as jnp
import numpy as np
from jax import lax
from jax.experimental import pallas as pl
from jax.experimental.pallas import tpu as pltpu
from jax.sharding import PartitionSpec as P

GATE_NORM = 16.0
NORM_EPS = 1e-06
LANES = 128


def rms_scale(values, scales):
    floats = values.astype(jnp.float32)
    return floats * lax.rsqrt(jnp.mean(floats * floats, axis=-1, keepdims=True) + NORM_EPS) * scales


def range_matrices(length):
    i = np.arange(length)[:, None]
    s = np.arange(length)[None, :]
    rows = []
    size = 2
    while size <= length:
        middle = i // size * size + size // 2
        late = i >= middle
        rows.append(np.where(late, (s >= middle) & (s <= i), (s >= i) & (s < middle)))
        rows.append(np.where(late, (s >= middle) & (s < i), (s > i) & (s < middle)))
        size *= 2
    return np.concatenate(rows, 0).astype(np.float32)


def attention_kernel(
    key_width, value_width, q_ref, k_ref, v_ref, g_ref, bias_ref, spike_ref, gain_ref, m_ref, o_ref
):
    length, lanes = q_ref.shape
    heads = lanes // key_width
    pre = g_ref[...] + bias_ref[...]
    log_sig = jnp.minimum(pre, 0.0) - jnp.log1p(jnp.exp(-jnp.abs(pre)))
    decay = log_sig / GATE_NORM + spike_ref[...]
    high = decay.astype(jnp.bfloat16)
    low = (decay - high.astype(jnp.float32)).astype(jnp.bfloat16)
    q = q_ref[...].astype(jnp.float32) * key_width ** (-0.5)
    k = k_ref[...].astype(jnp.float32)
    lane_head = lax.broadcasted_iota(jnp.int32, (length, lanes), 1) // key_width
    apart = lax.broadcasted_iota(jnp.int32, (length, length), 0) ^ lax.broadcasted_iota(
        jnp.int32, (length, length), 1
    )

    def scores(left, right, h):
        masked = jnp.where(lane_head == h, left, 0.0).astype(jnp.bfloat16)
        return lax.dot_general(
            masked, right, (((1,), (1,)), ((), ())), preferred_element_type=jnp.float32
        )

    def factor(index):
        part = m_ref[pl.ds(index * length, length), :]
        total = jnp.dot(part, high, preferred_element_type=jnp.float32)
        return jnp.exp(total + jnp.dot(part, low, preferred_element_type=jnp.float32))

    k_low = k.astype(jnp.bfloat16)
    acc = [2.0 * scores(q, k_low, h) for h in range(heads)]
    level, size = 0, 1
    while size < length:
        left = q * factor(2 * level)
        right = (k * factor(2 * level + 1)).astype(jnp.bfloat16)
        acc = [jnp.where(apart >= size, scores(left, right, h), acc[h]) for h in range(heads)]
        level, size = level + 1, size * 2
    per = min(heads, max(1, LANES // value_width))
    wide = per * value_width
    lane_value = lax.broadcasted_iota(jnp.int32, (length, wide), 1) // value_width
    for group in range(heads // per):
        span = slice(group * wide, (group + 1) * wide)
        values = v_ref[:, span]
        mixed = jnp.zeros((length, wide), jnp.float32)
        for n in range(per):
            one = jnp.dot(
                acc[group * per + n].astype(jnp.bfloat16), values, preferred_element_type=jnp.float32
            )
            mixed = jnp.where(lane_value == n, one, mixed)
        square = mixed * mixed
        scale = jnp.zeros((length, wide), jnp.float32)
        for n in range(per):
            mean = jnp.sum(jnp.where(lane_value == n, square, 0.0), -1, keepdims=True) / value_width
            scale = jnp.where(lane_value == n, lax.rsqrt(mean + NORM_EPS), scale)
        o_ref[:, span] = (mixed * scale * gain_ref[:, span]).astype(jnp.bfloat16)


def attention(length, key_width, value_width, q, k, v, gate, bias, spike, gain):
    rows, width = q.shape
    lanes = min(width, LANES)
    wide = lanes // key_width * value_width
    matrices = jnp.asarray(range_matrices(length), jnp.bfloat16)
    narrow_spec = pl.BlockSpec((length, lanes), lambda s, g: (s, g))
    wide_spec = pl.BlockSpec((length, wide), lambda s, g: (s, g))
    return pl.pallas_call(
        functools.partial(attention_kernel, key_width, value_width),
        grid=(rows // length, width // lanes),
        in_specs=[
            narrow_spec,
            narrow_spec,
            wide_spec,
            narrow_spec,
            pl.BlockSpec((1, lanes), lambda s, g: (0, g)),
            narrow_spec,
            pl.BlockSpec((1, wide), lambda s, g: (0, 0)),
            pl.BlockSpec(matrices.shape, lambda s, g: (0, 0)),
        ],
        out_specs=wide_spec,
        out_shape=jax.ShapeDtypeStruct(v.shape, jnp.bfloat16),
    )(q, k, v, gate, bias, spike, gain, matrices)


def make_shards(n_fs, n_tp):
    half_ring = n_fs // 2
    order = [2 * i for i in range(half_ring)] + [2 * i + 1 for i in reversed(range(half_ring))]
    ahead = [(order[i], order[(i + 1) % n_fs]) for i in range(n_fs)]
    behind = [(b, a) for a, b in ahead]
    swap = [(0, 1), (1, 0)]

    def position(f):
        return jnp.where(f % 2 == 0, f // 2, n_fs - 1 - f // 2)

    def member(p):
        return jnp.where(p < half_ring, 2 * p, 2 * (n_fs - 1 - p) + 1)

    def ring(block):
        out, back, front = [block], block, block
        for _ in range(half_ring - 1):
            back = lax.ppermute(back, "fs", ahead)
            front = lax.ppermute(front, "fs", behind)
            out += [back, front]
        cut = block.shape[0] // 2
        back = lax.ppermute(back[:cut], "fs", ahead)
        front = lax.ppermute(front[cut:], "fs", behind)
        return out + [jnp.concatenate([back, front], 0)]

    def tp_scatter(total):
        if n_tp != 2:
            return lax.psum_scatter(
                total.astype(jnp.bfloat16), "tp", scatter_dimension=1, tiled=True
            ).astype(jnp.float32)
        c = lax.axis_index("tp")
        cut = total.shape[1] // 2
        mine = lax.dynamic_slice_in_dim(total, c * cut, cut, 1)
        other = lax.dynamic_slice_in_dim(total, (1 - c) * cut, cut, 1)
        return mine + lax.ppermute(other.astype(jnp.bfloat16), "tp", swap).astype(jnp.float32)

    def tp_gather(part):
        if n_tp != 2:
            return lax.all_gather(part, "tp", axis=1, tiled=True)
        other = lax.ppermute(part, "tp", swap)
        first = lax.axis_index("tp") == 0
        return jnp.concatenate([jnp.where(first, part, other), jnp.where(first, other, part)], 1)

    def shards(
        tokens,
        attention_norm_gain,
        query_weight,
        key_weight,
        value_weight,
        decay_weight,
        decay_gate_bias,
        decay_spike_extra,
        head_output_gain,
        output_weight,
        channel_norm_gain,
        gate_weight,
        up_weight,
        down_weight,
    ):
        r, f, c = lax.axis_index("rep"), lax.axis_index("fs"), lax.axis_index("tp")
        length, model = tokens.shape
        block = model // n_fs
        p = position(f)

        def own(weight, which=None, axis=1):
            cut = weight.shape[axis] // 2
            return lax.dynamic_slice_in_dim(weight, (r if which is None else which) * cut, cut, axis)

        shifts = [0]
        for d in range(1, half_ring):
            shifts += [n_fs - d, d]
        shifts += [half_ring]
        slots = [member((p + d) % n_fs) for d in shifts]

        def ring_order(array):
            axis = array.ndim - 1
            return jnp.concatenate(
                [lax.dynamic_slice_in_dim(array, s * block, block, axis) for s in slots], axis
            )

        def natural_order(array):
            pieces = []
            for j in range(n_fs):
                d = (order.index(j) - p) % n_fs
                slot = jnp.where(d > half_ring, 2 * (n_fs - d) - 1, 2 * d)
                slot = jnp.where(d == half_ring, n_fs - 1, slot)
                pieces.append(lax.dynamic_slice_in_dim(array, slot * block, block, 1))
            return jnp.concatenate(pieces, 1)

        def over_blocks(rows, blocks):
            total = None
            for s, weight in enumerate(blocks):
                term = jnp.dot(
                    rows[:, s * block : (s + 1) * block], weight, preferred_element_type=jnp.float32
                )
                total = term if total is None else total + term
            return total

        def to_features(rows, blocks):
            return jnp.concatenate(
                [
                    lax.dot_general(
                        rows, w, (((1,), (1,)), ((), ())), preferred_element_type=jnp.float32
                    )
                    for w in blocks
                ],
                1,
            )

        narrow = query_weight.shape[1] // 2
        wide = value_weight.shape[1] // 2
        heads = decay_spike_extra.shape[1] // 2
        key_width, value_width = narrow // heads, wide // heads
        first = ring(
            jnp.concatenate(
                [own(query_weight), own(key_weight), own(value_weight), own(decay_weight)], 1
            )
        )
        hidden_width = gate_weight.shape[1] // 2
        second = ring(jnp.concatenate([own(output_weight), own(gate_weight), own(up_weight)], 1))
        third = ring(own(down_weight))

        mine = ring_order(tokens)
        both = jnp.concatenate([mine, lax.ppermute(mine, "rep", swap)], 0)
        spike = jnp.concatenate(
            [
                own(decay_spike_extra),
                lax.ppermute(own(decay_spike_extra, 1 - r), "rep", swap),
            ],
            0,
        )
        spike = jnp.repeat(spike, key_width, axis=1)
        bias = own(decay_gate_bias, axis=0)[None, :]
        group_heads = min(narrow, LANES) // key_width
        head_gain = jnp.tile(head_output_gain, group_heads)[None, :]

        normed = rms_scale(both, ring_order(attention_norm_gain)).astype(jnp.bfloat16)
        proj = over_blocks(normed, first)
        low = proj[:, : 2 * narrow + wide].astype(jnp.bfloat16)
        attended = attention(
            length,
            key_width,
            value_width,
            low[:, :narrow],
            low[:, narrow : 2 * narrow],
            low[:, 2 * narrow :],
            proj[:, 2 * narrow + wide :],
            bias,
            spike,
            head_gain,
        )
        mixer = tp_scatter(to_features(attended, [w[:, :wide] for w in second]))
        mixer = mixer.astype(jnp.bfloat16)
        turned = jnp.concatenate([mixer[length:], mixer[:length]], 0)
        mixed = mixer.astype(jnp.float32) + lax.ppermute(turned, "rep", swap).astype(jnp.float32)
        part = mixed.shape[1]
        residual_part = (
            lax.dynamic_slice_in_dim(both, c * part, part, 1).astype(jnp.float32) + mixed
        ).astype(jnp.bfloat16)
        residual = tp_gather(residual_part)
        normed_two = rms_scale(residual, ring_order(channel_norm_gain)).astype(jnp.bfloat16)
        pre = over_blocks(normed_two, [w[:, wide:] for w in second])
        hidden = (jax.nn.silu(pre[:, :hidden_width]) * pre[:, hidden_width:]).astype(jnp.bfloat16)
        channel = tp_scatter(to_features(hidden, third)).astype(jnp.bfloat16)
        other = lax.ppermute(channel[length:], "rep", swap).astype(jnp.float32)
        channel = channel[:length].astype(jnp.float32) + other
        out_part = (residual_part[:length].astype(jnp.float32) + channel).astype(jnp.bfloat16)
        return natural_order(tp_gather(out_part))

    return shards


def solution(mesh):
    in_specs = (
        P(("rep", "fs"), None),
        P(),
        P("fs", "tp"),
        P("fs", "tp"),
        P("fs", "tp"),
        P("fs", "tp"),
        P("tp"),
        P(("rep", "fs"), "tp"),
        P(),
        P("fs", "tp"),
        P(),
        P("fs", "tp"),
        P("fs", "tp"),
        P("fs", "tp"),
    )
    return jax.shard_map(
        make_shards(mesh.shape["fs"], mesh.shape["tp"]),
        mesh=mesh,
        in_specs=in_specs,
        out_specs=P(("rep", "fs"), None),
        check_vma=False,
    )
```

```python
import functools

import jax
import jax.numpy as jnp
import numpy as np
from jax import lax
from jax.experimental import pallas as pl
from jax.sharding import PartitionSpec as P

GATE_NORM = 16.0
NORM_EPS = 1e-06
LANES = 128


def rms_scale(values, scales):
    floats = values.astype(jnp.float32)
    return floats * lax.rsqrt(jnp.mean(floats * floats, axis=-1, keepdims=True) + NORM_EPS) * scales


def range_matrices(length):
    i = np.arange(length)[:, None]
    s = np.arange(length)[None, :]
    rows = []
    size = 2
    while size <= length:
        middle = i // size * size + size // 2
        late = i >= middle
        rows.append(np.where(late, (s >= middle) & (s <= i), (s >= i) & (s < middle)))
        rows.append(np.where(late, (s >= middle) & (s < i), (s > i) & (s < middle)))
        size *= 2
    return np.concatenate(rows, 0).astype(np.float32)


def attention_kernel(
    key_width, value_width, q_ref, k_ref, v_ref, g_ref, bias_ref, spike_ref, gain_ref, m_ref, o_ref
):
    length, lanes = q_ref.shape
    heads = lanes // key_width
    pre = g_ref[...] + bias_ref[...]
    log_sig = jnp.minimum(pre, 0.0) - jnp.log1p(jnp.exp(-jnp.abs(pre)))
    decay = log_sig / GATE_NORM + spike_ref[...]
    high = decay.astype(jnp.bfloat16)
    low = (decay - high.astype(jnp.float32)).astype(jnp.bfloat16)
    q = q_ref[...].astype(jnp.float32) * key_width ** (-0.5)
    k = k_ref[...].astype(jnp.float32)
    lane_head = lax.broadcasted_iota(jnp.int32, (length, lanes), 1) // key_width
    apart = lax.broadcasted_iota(jnp.int32, (length, length), 0) ^ lax.broadcasted_iota(
        jnp.int32, (length, length), 1
    )

    def scores(left, right, h):
        masked = jnp.where(lane_head == h, left, 0.0).astype(jnp.bfloat16)
        return lax.dot_general(
            masked, right, (((1,), (1,)), ((), ())), preferred_element_type=jnp.float32
        )

    def factor(index):
        part = m_ref[pl.ds(index * length, length), :]
        total = jnp.dot(part, high, preferred_element_type=jnp.float32)
        return jnp.exp(total + jnp.dot(part, low, preferred_element_type=jnp.float32))

    k_low = k.astype(jnp.bfloat16)
    acc = [2.0 * scores(q, k_low, h) for h in range(heads)]
    level, size = 0, 1
    while size < length:
        left = q * factor(2 * level)
        right = (k * factor(2 * level + 1)).astype(jnp.bfloat16)
        acc = [jnp.where(apart >= size, scores(left, right, h), acc[h]) for h in range(heads)]
        level, size = level + 1, size * 2
    per = min(heads, max(1, LANES // value_width))
    wide = per * value_width
    lane_value = lax.broadcasted_iota(jnp.int32, (length, wide), 1) // value_width
    for group in range(heads // per):
        span = slice(group * wide, (group + 1) * wide)
        values = v_ref[:, span]
        mixed = jnp.zeros((length, wide), jnp.float32)
        for n in range(per):
            one = jnp.dot(
                acc[group * per + n].astype(jnp.bfloat16), values, preferred_element_type=jnp.float32
            )
            mixed = jnp.where(lane_value == n, one, mixed)
        square = mixed * mixed
        scale = jnp.zeros((length, wide), jnp.float32)
        for n in range(per):
            mean = jnp.sum(jnp.where(lane_value == n, square, 0.0), -1, keepdims=True) / value_width
            scale = jnp.where(lane_value == n, lax.rsqrt(mean + NORM_EPS), scale)
        o_ref[:, span] = (mixed * scale * gain_ref[:, span]).astype(jnp.bfloat16)


def attention(length, key_width, value_width, q, k, v, gate, bias, spike, gain):
    rows, width = q.shape
    lanes = min(width, LANES)
    wide = lanes // key_width * value_width
    matrices = jnp.asarray(range_matrices(length), jnp.bfloat16)
    narrow_spec = pl.BlockSpec((length, lanes), lambda s, g: (s, g))
    wide_spec = pl.BlockSpec((length, wide), lambda s, g: (s, g))
    return pl.pallas_call(
        functools.partial(attention_kernel, key_width, value_width),
        grid=(rows // length, width // lanes),
        in_specs=[
            narrow_spec,
            narrow_spec,
            wide_spec,
            narrow_spec,
            pl.BlockSpec((1, lanes), lambda s, g: (0, g)),
            narrow_spec,
            pl.BlockSpec((1, wide), lambda s, g: (0, 0)),
            pl.BlockSpec(matrices.shape, lambda s, g: (0, 0)),
        ],
        out_specs=wide_spec,
        out_shape=jax.ShapeDtypeStruct(v.shape, jnp.bfloat16),
    )(q, k, v, gate, bias, spike, gain, matrices)


def make_shards(n_fs, n_tp):
    half_ring = n_fs // 2
    order = [2 * i for i in range(half_ring)] + [2 * i + 1 for i in reversed(range(half_ring))]
    ahead = [(order[i], order[(i + 1) % n_fs]) for i in range(n_fs)]
    behind = [(b, a) for a, b in ahead]
    swap = [(0, 1), (1, 0)]

    def position(f):
        return jnp.where(f % 2 == 0, f // 2, n_fs - 1 - f // 2)

    def member(p):
        return jnp.where(p < half_ring, 2 * p, 2 * (n_fs - 1 - p) + 1)

    def ring(block):
        out, back, front = [block], block, block
        for _ in range(1, half_ring):
            back = lax.ppermute(back, "fs", ahead)
            front = lax.ppermute(front, "fs", behind)
            out += [back, front]
        cut = block.shape[0] // 2
        back = lax.ppermute(back[:cut], "fs", ahead)
        front = lax.ppermute(front[cut:], "fs", behind)
        return out + [jnp.concatenate([back, front], 0)]

    def tp_scatter(total):
        if n_tp != 2:
            return lax.psum_scatter(
                total.astype(jnp.bfloat16), "tp", scatter_dimension=1, tiled=True
            ).astype(jnp.float32)
        c = lax.axis_index("tp")
        cut = total.shape[1] // 2
        mine = lax.dynamic_slice_in_dim(total, c * cut, cut, 1)
        other = lax.dynamic_slice_in_dim(total, (1 - c) * cut, cut, 1)
        return mine + lax.ppermute(other.astype(jnp.bfloat16), "tp", swap).astype(jnp.float32)

    def tp_gather(part):
        if n_tp != 2:
            return lax.all_gather(part, "tp", axis=1, tiled=True)
        other = lax.ppermute(part, "tp", swap)
        first = lax.axis_index("tp") == 0
        return jnp.concatenate([jnp.where(first, part, other), jnp.where(first, other, part)], 1)

    def shards(
        tokens,
        attention_norm_gain,
        query_weight,
        key_weight,
        value_weight,
        decay_weight,
        decay_gate_bias,
        decay_spike_extra,
        head_output_gain,
        output_weight,
        channel_norm_gain,
        gate_weight,
        up_weight,
        down_weight,
    ):
        r, f, c = lax.axis_index("rep"), lax.axis_index("fs"), lax.axis_index("tp")
        length, model = tokens.shape
        block = model // n_fs
        p = position(f)

        def own(weight, which=None, axis=1):
            cut = weight.shape[axis] // 2
            return lax.dynamic_slice_in_dim(weight, (r if which is None else which) * cut, cut, axis)

        shifts = [0]
        for d in range(1, half_ring):
            shifts += [n_fs - d, d]
        shifts += [half_ring]
        slots = [member((p + d) % n_fs) for d in shifts]

        def ring_order(array):
            axis = array.ndim - 1
            return jnp.concatenate(
                [lax.dynamic_slice_in_dim(array, s * block, block, axis) for s in slots], axis
            )

        def natural_order(array):
            pieces = []
            for j in range(n_fs):
                d = (order.index(j) - p) % n_fs
                slot = jnp.where(d > half_ring, 2 * (n_fs - d) - 1, 2 * d)
                slot = jnp.where(d == half_ring, n_fs - 1, slot)
                pieces.append(lax.dynamic_slice_in_dim(array, slot * block, block, 1))
            return jnp.concatenate(pieces, 1)

        def over_blocks(rows, blocks):
            total = None
            for s, weight in enumerate(blocks):
                term = jnp.dot(
                    rows[:, s * block : (s + 1) * block], weight, preferred_element_type=jnp.float32
                )
                total = term if total is None else total + term
            return total

        def to_features(rows, blocks):
            return jnp.concatenate(
                [
                    lax.dot_general(
                        rows, w, (((1,), (1,)), ((), ())), preferred_element_type=jnp.float32
                    )
                    for w in blocks
                ],
                1,
            )

        narrow = query_weight.shape[1] // 2
        wide = value_weight.shape[1] // 2
        heads = decay_spike_extra.shape[1] // 2
        key_width, value_width = narrow // heads, wide // heads
        first = ring(
            jnp.concatenate(
                [own(query_weight), own(key_weight), own(value_weight), own(decay_weight)], 1
            ),
        )
        outputs = ring(own(output_weight))
        gates = ring(own(gate_weight))
        ups = ring(own(up_weight))
        downs = ring(own(down_weight))

        mine = ring_order(tokens)
        both = jnp.concatenate([mine, lax.ppermute(mine, "rep", swap)], 0)
        spike = jnp.concatenate(
            [
                own(decay_spike_extra),
                lax.ppermute(own(decay_spike_extra, 1 - r), "rep", swap),
            ],
            0,
        )
        spike = jnp.repeat(spike, key_width, axis=1)
        bias = own(decay_gate_bias, axis=0)[None, :]
        group_heads = min(narrow, LANES) // key_width
        head_gain = jnp.tile(head_output_gain, group_heads)[None, :]

        normed = rms_scale(both, ring_order(attention_norm_gain)).astype(jnp.bfloat16)
        proj = over_blocks(normed, first)
        low = proj[:, : 2 * narrow + wide].astype(jnp.bfloat16)
        attended = attention(
            length,
            key_width,
            value_width,
            low[:, :narrow],
            low[:, narrow : 2 * narrow],
            low[:, 2 * narrow :],
            proj[:, 2 * narrow + wide :],
            bias,
            spike,
            head_gain,
        )
        mixer = tp_scatter(to_features(attended, outputs)).astype(jnp.bfloat16)
        turned = jnp.concatenate([mixer[length:], mixer[:length]], 0)
        turned = lax.ppermute(turned, "rep", swap)
        mixed = mixer.astype(jnp.float32) + turned.astype(jnp.float32)
        part = mixed.shape[1]
        residual_part = (
            lax.dynamic_slice_in_dim(both, c * part, part, 1).astype(jnp.float32) + mixed
        ).astype(jnp.bfloat16)
        residual = tp_gather(residual_part)
        normed_two = rms_scale(residual, ring_order(channel_norm_gain)).astype(jnp.bfloat16)
        gate_pre = over_blocks(normed_two, gates)
        up_pre = over_blocks(normed_two, ups)
        hidden = (jax.nn.silu(gate_pre) * up_pre).astype(jnp.bfloat16)
        split = n_fs - 3
        pieces = []
        for low_slot, high_slot in ((0, split), (split, n_fs)):
            channel = tp_scatter(to_features(hidden, downs[low_slot:high_slot]))
            channel = channel.astype(jnp.bfloat16)
            cut = channel.shape[1]
            other = lax.ppermute(channel[length:], "rep", swap).astype(jnp.float32)
            channel = channel[:length].astype(jnp.float32) + other
            start = low_slot * block + c * cut
            rest = lax.dynamic_slice_in_dim(residual[:length], start, cut, 1).astype(jnp.float32)
            pieces.append(tp_gather((rest + channel).astype(jnp.bfloat16)))
        return natural_order(jnp.concatenate(pieces, 1))

    return shards


def solution(mesh):
    in_specs = (
        P(("rep", "fs"), None),
        P(),
        P("fs", "tp"),
        P("fs", "tp"),
        P("fs", "tp"),
        P("fs", "tp"),
        P("tp"),
        P(("rep", "fs"), "tp"),
        P(),
        P("fs", "tp"),
        P(),
        P("fs", "tp"),
        P("fs", "tp"),
        P("fs", "tp"),
    )
    shards = make_shards(mesh.shape["fs"], mesh.shape["tp"])

    return jax.shard_map(
        shards,
        mesh=mesh,
        in_specs=in_specs,
        out_specs=P(("rep", "fs"), None),
        check_vma=False,
    )
```

```python
import functools

import jax
import jax.numpy as jnp
import numpy as np
from jax import lax
from jax.experimental import pallas as pl
from jax.sharding import PartitionSpec as P

GATE_NORM = 16.0
NORM_EPS = 1e-06
LANES = 128


def rms_scale(values, scales):
    floats = values.astype(jnp.float32)
    return floats * lax.rsqrt(jnp.mean(floats * floats, axis=-1, keepdims=True) + NORM_EPS) * scales


def range_matrices(length):
    i = np.arange(length)[:, None]
    s = np.arange(length)[None, :]
    rows = []
    size = 2
    while size <= length:
        middle = i // size * size + size // 2
        late = i >= middle
        rows.append(np.where(late, (s >= middle) & (s <= i), (s >= i) & (s < middle)))
        rows.append(np.where(late, (s >= middle) & (s < i), (s > i) & (s < middle)))
        size *= 2
    return np.concatenate(rows, 0).astype(np.float32)


def attention_kernel(
    key_width, value_width, q_ref, k_ref, v_ref, g_ref, bias_ref, spike_ref, gain_ref, m_ref, o_ref
):
    length, lanes = q_ref.shape
    heads = lanes // key_width
    pre = g_ref[...] + bias_ref[...]
    log_sig = jnp.minimum(pre, 0.0) - jnp.log1p(jnp.exp(-jnp.abs(pre)))
    decay = log_sig / GATE_NORM + spike_ref[...]
    high = decay.astype(jnp.bfloat16)
    low = (decay - high.astype(jnp.float32)).astype(jnp.bfloat16)
    q = q_ref[...].astype(jnp.float32) * key_width ** (-0.5)
    k = k_ref[...].astype(jnp.float32)
    lane_head = lax.broadcasted_iota(jnp.int32, (length, lanes), 1) // key_width
    apart = lax.broadcasted_iota(jnp.int32, (length, length), 0) ^ lax.broadcasted_iota(
        jnp.int32, (length, length), 1
    )

    def scores(left, right, h):
        masked = jnp.where(lane_head == h, left, 0.0).astype(jnp.bfloat16)
        return lax.dot_general(
            masked, right, (((1,), (1,)), ((), ())), preferred_element_type=jnp.float32
        )

    def factor(index):
        part = m_ref[pl.ds(index * length, length), :]
        total = jnp.dot(part, high, preferred_element_type=jnp.float32)
        return jnp.exp(total + jnp.dot(part, low, preferred_element_type=jnp.float32))

    k_low = k.astype(jnp.bfloat16)
    acc = [2.0 * scores(q, k_low, h) for h in range(heads)]
    level, size = 0, 1
    while size < length:
        left = q * factor(2 * level)
        right = (k * factor(2 * level + 1)).astype(jnp.bfloat16)
        acc = [jnp.where(apart >= size, scores(left, right, h), acc[h]) for h in range(heads)]
        level, size = level + 1, size * 2
    per = min(heads, max(1, LANES // value_width))
    wide = per * value_width
    lane_value = lax.broadcasted_iota(jnp.int32, (length, wide), 1) // value_width
    for group in range(heads // per):
        span = slice(group * wide, (group + 1) * wide)
        values = v_ref[:, span]
        mixed = jnp.zeros((length, wide), jnp.float32)
        for n in range(per):
            one = jnp.dot(
                acc[group * per + n].astype(jnp.bfloat16), values, preferred_element_type=jnp.float32
            )
            mixed = jnp.where(lane_value == n, one, mixed)
        square = mixed * mixed
        scale = jnp.zeros((length, wide), jnp.float32)
        for n in range(per):
            mean = jnp.sum(jnp.where(lane_value == n, square, 0.0), -1, keepdims=True) / value_width
            scale = jnp.where(lane_value == n, lax.rsqrt(mean + NORM_EPS), scale)
        o_ref[:, span] = (mixed * scale * gain_ref[:, span]).astype(jnp.bfloat16)


def attention(length, key_width, value_width, q, k, v, gate, bias, spike, gain):
    rows, width = q.shape
    lanes = min(width, LANES)
    wide = lanes // key_width * value_width
    matrices = jnp.asarray(range_matrices(length), jnp.bfloat16)
    narrow_spec = pl.BlockSpec((length, lanes), lambda s, g: (s, g))
    wide_spec = pl.BlockSpec((length, wide), lambda s, g: (s, g))
    return pl.pallas_call(
        functools.partial(attention_kernel, key_width, value_width),
        grid=(rows // length, width // lanes),
        in_specs=[
            narrow_spec,
            narrow_spec,
            wide_spec,
            narrow_spec,
            pl.BlockSpec((1, lanes), lambda s, g: (0, g)),
            narrow_spec,
            pl.BlockSpec((1, wide), lambda s, g: (0, 0)),
            pl.BlockSpec(matrices.shape, lambda s, g: (0, 0)),
        ],
        out_specs=wide_spec,
        out_shape=jax.ShapeDtypeStruct(v.shape, jnp.bfloat16),
    )(q, k, v, gate, bias, spike, gain, matrices)


def make_shards(n_fs, n_tp):
    half_ring = n_fs // 2
    order = [2 * i for i in range(half_ring)] + [2 * i + 1 for i in reversed(range(half_ring))]
    ahead = [(order[i], order[(i + 1) % n_fs]) for i in range(n_fs)]
    behind = [(b, a) for a, b in ahead]
    swap = [(0, 1), (1, 0)]

    def position(f):
        return jnp.where(f % 2 == 0, f // 2, n_fs - 1 - f // 2)

    def member(p):
        return jnp.where(p < half_ring, 2 * p, 2 * (n_fs - 1 - p) + 1)

    def ring(block):
        out, back, front = [block], block, block
        for _ in range(1, half_ring):
            back = lax.ppermute(back, "fs", ahead)
            front = lax.ppermute(front, "fs", behind)
            out += [back, front]
        cut = block.shape[0] // 2
        back = lax.ppermute(back[:cut], "fs", ahead)
        front = lax.ppermute(front[cut:], "fs", behind)
        return out + [jnp.concatenate([back, front], 0)]

    def halves_ring(block, names):
        cut = block.shape[0] // 2
        parts = []
        for name, part in zip(names, (block[:cut], block[cut:])):
            out, back, front = [part], part, part
            for step in range(1, half_ring + 1):
                if step < half_ring or name == names[0]:
                    back = lax.ppermute(back, "fs", ahead)
                if step < half_ring or name == names[1]:
                    front = lax.ppermute(front, "fs", behind)
                if step < half_ring:
                    out += [back, front]
            parts.append(out + [back if name == names[0] else front])
        return [half for pair in zip(*parts) for half in pair]

    def tp_scatter(total):
        if n_tp != 2:
            return lax.psum_scatter(
                total.astype(jnp.bfloat16), "tp", scatter_dimension=1, tiled=True
            ).astype(jnp.float32)
        c = lax.axis_index("tp")
        cut = total.shape[1] // 2
        mine = lax.dynamic_slice_in_dim(total, c * cut, cut, 1)
        other = lax.dynamic_slice_in_dim(total, (1 - c) * cut, cut, 1)
        return mine + lax.ppermute(other.astype(jnp.bfloat16), "tp", swap).astype(jnp.float32)

    def tp_gather(part):
        if n_tp != 2:
            return lax.all_gather(part, "tp", axis=1, tiled=True)
        other = lax.ppermute(part, "tp", swap)
        first = lax.axis_index("tp") == 0
        return jnp.concatenate([jnp.where(first, part, other), jnp.where(first, other, part)], 1)

    def shards(
        tokens,
        attention_norm_gain,
        query_weight,
        key_weight,
        value_weight,
        decay_weight,
        decay_gate_bias,
        decay_spike_extra,
        head_output_gain,
        output_weight,
        channel_norm_gain,
        gate_weight,
        up_weight,
        down_weight,
    ):
        r, f, c = lax.axis_index("rep"), lax.axis_index("fs"), lax.axis_index("tp")
        length, model = tokens.shape
        block = model // n_fs
        p = position(f)

        def own(weight, which=None, axis=1):
            cut = weight.shape[axis] // 2
            return lax.dynamic_slice_in_dim(weight, (r if which is None else which) * cut, cut, axis)

        shifts = [0]
        for d in range(1, half_ring):
            shifts += [n_fs - d, d]
        shifts += [half_ring]
        slots = [member((p + d) % n_fs) for d in shifts]

        def ring_order(array):
            axis = array.ndim - 1
            return jnp.concatenate(
                [lax.dynamic_slice_in_dim(array, s * block, block, axis) for s in slots], axis
            )

        def natural_order(array):
            pieces = []
            for j in range(n_fs):
                d = (order.index(j) - p) % n_fs
                slot = jnp.where(d > half_ring, 2 * (n_fs - d) - 1, 2 * d)
                slot = jnp.where(d == half_ring, n_fs - 1, slot)
                pieces.append(lax.dynamic_slice_in_dim(array, slot * block, block, 1))
            return jnp.concatenate(pieces, 1)

        def over_blocks(rows, blocks):
            total = None
            for s, weight in enumerate(blocks):
                term = jnp.dot(
                    rows[:, s * block : (s + 1) * block],
                    weight,
                    preferred_element_type=jnp.float32,
                )
                total = term if total is None else total + term
            return total

        def to_features(rows, blocks):
            terms = []
            for weight in blocks:
                terms.append(
                    lax.dot_general(
                        rows, weight, (((1,), (1,)), ((), ())), preferred_element_type=jnp.float32
                    )
                )
            return jnp.concatenate(terms, 1)

        narrow = query_weight.shape[1] // 2
        wide = value_weight.shape[1] // 2
        heads = decay_spike_extra.shape[1] // 2
        key_width, value_width = narrow // heads, wide // heads
        first = ring(
            jnp.concatenate(
                [own(query_weight), own(key_weight), own(value_weight), own(decay_weight)], 1
            ),
        )
        outputs = ring(own(output_weight))
        gates = ring(own(gate_weight))
        ups = ring(own(up_weight))
        downs = halves_ring(own(down_weight), "dh")

        mine = ring_order(tokens)
        both = jnp.concatenate([mine, lax.ppermute(mine, "rep", swap)], 0)
        spike = jnp.concatenate(
            [
                own(decay_spike_extra),
                lax.ppermute(own(decay_spike_extra, 1 - r), "rep", swap),
            ],
            0,
        )
        spike = jnp.repeat(spike, key_width, axis=1)
        bias = own(decay_gate_bias, axis=0)[None, :]
        group_heads = min(narrow, LANES) // key_width
        head_gain = jnp.tile(head_output_gain, group_heads)[None, :]

        normed = rms_scale(both, ring_order(attention_norm_gain)).astype(jnp.bfloat16)
        proj = over_blocks(normed, first)
        low = proj[:, : 2 * narrow + wide].astype(jnp.bfloat16)
        attended = attention(
            length,
            key_width,
            value_width,
            low[:, :narrow],
            low[:, narrow : 2 * narrow],
            low[:, 2 * narrow :],
            proj[:, 2 * narrow + wide :],
            bias,
            spike,
            head_gain,
        )
        mixer = to_features(attended, outputs)
        mixer = tp_scatter(mixer).astype(jnp.bfloat16)
        turned = jnp.concatenate([mixer[length:], mixer[:length]], 0)
        turned = lax.ppermute(turned, "rep", swap)
        part = mixer.shape[1]
        mixed = mixer.astype(jnp.float32) + turned.astype(jnp.float32)
        residual_part = (
            lax.dynamic_slice_in_dim(both, c * part, part, 1).astype(jnp.float32) + mixed
        ).astype(jnp.bfloat16)
        residual = tp_gather(residual_part)
        normed_two = rms_scale(residual, ring_order(channel_norm_gain)).astype(jnp.bfloat16)
        gate_pre = over_blocks(normed_two, gates)
        up_pre = over_blocks(normed_two, ups)
        hidden = (jax.nn.silu(gate_pre) * up_pre).astype(jnp.bfloat16)
        split = n_fs - 3
        pieces = []
        for low_slot, high_slot in ((0, split), (split, n_fs)):
            channel = tp_scatter(to_features(hidden, downs[2 * low_slot : 2 * high_slot]))
            channel = channel.astype(jnp.bfloat16)
            cut = channel.shape[1]
            other = lax.ppermute(channel[length:], "rep", swap).astype(jnp.float32)
            channel = channel[:length].astype(jnp.float32) + other
            start = low_slot * block + c * cut
            rest = lax.dynamic_slice_in_dim(residual[:length], start, cut, 1).astype(jnp.float32)
            pieces.append(tp_gather((rest + channel).astype(jnp.bfloat16)))
        return natural_order(jnp.concatenate(pieces, 1))

    return shards


def solution(mesh):
    in_specs = (
        P(("rep", "fs"), None),
        P(),
        P("fs", "tp"),
        P("fs", "tp"),
        P("fs", "tp"),
        P("fs", "tp"),
        P("tp"),
        P(("rep", "fs"), "tp"),
        P(),
        P("fs", "tp"),
        P(),
        P("fs", "tp"),
        P("fs", "tp"),
        P("fs", "tp"),
    )
    shards = make_shards(mesh.shape["fs"], mesh.shape["tp"])

    return jax.shard_map(
        shards,
        mesh=mesh,
        in_specs=in_specs,
        out_specs=P(("rep", "fs"), None),
        check_vma=False,
    )
```
